32 devices in a mesh: dp: 4 (over y, x), kv: 4 (over z), tp: 2 (over core).
Axes of the slice: x: 2, y: 2, z: 4, core: 2. Of those that a mesh axis runs over, the one named last changes fastest.
Arguments:
- tokens: bfloat16 [32, 4096], P('dp', 'kv'), parts along dimension 0, may hold values from -16 to 16
- gain_mix: float32 [4096], P('kv'), may hold values from 0.1 to 1.9
- w_query: bfloat16 [4096, 2048], P('kv', 'tp'), may hold values from -0.09375 to 0.09375
- w_key: bfloat16 [4096, 2048], P('kv', 'tp'), may hold values from -0.09375 to 0.09375
- w_value: bfloat16 [4096, 2048], P('kv', 'tp'), may hold values from -0.09375 to 0.09375
- w_igate: bfloat16 [4096, 16], P('kv', 'tp'), may hold values from -0.09375 to 0.09375
- w_fgate: bfloat16 [4096, 16], P('kv', 'tp'), may hold values from -0.09375 to 0.09375
- bias_igate: float32 [16], P('tp'), may hold values from -1 to 1
- bias_fgate: float32 [16], P('tp'), may hold values from -1 to 4
- memory: float32 [32, 16, 128, 128], P(('dp', 'kv'), 'tp'), parts along dimension 0, may hold values from -0.8 to 0.8
- normalizer: float32 [32, 16, 128], P(('dp', 'kv'), 'tp'), parts along dimension 0, may hold values from -0.8 to 0.8
- stabilizer: float32 [32, 16], P(('dp', 'kv'), 'tp'), parts along dimension 0, may hold values from -1.5 to 1.5
- w_output: bfloat16 [2048, 4096], P('tp', 'kv'), may hold values from -0.125 to 0.125
- gain_mlp: float32 [4096], replicated, may hold values from 0.1 to 1.9
- w_gate: bfloat16 [4096, 11264], P(None, ('kv', 'tp')), may hold values from -0.09375 to 0.09375
- w_up: bfloat16 [4096, 11264], P(None, ('kv', 'tp')), may hold values from -0.09375 to 0.09375
- w_down: bfloat16 [11264, 4096], P(('kv', 'tp')), may hold values from -0.078125 to 0.078125
Outputs:
- mixed: bfloat16 [32, 4096], P('dp', ('kv', 'tp')), parts along dimension 0
- memory_next: float32 [32, 16, 128, 128], P(('dp', 'kv'), 'tp'), parts along dimension 0
- normalizer_next: float32 [32, 16, 128], P(('dp', 'kv'), 'tp'), parts along dimension 0
- stabilizer_next: float32 [32, 16], P(('dp', 'kv'), 'tp'), parts along dimension 0
The draws below stay inside these ranges and needn't reach their ends.
There are 4 independent parts, one for each index of `dp`. The reference program is written for one: setup_inputs(seed, part) draws one part's arguments, and reference() takes and returns one part's arrays. A program takes and returns all parts, laid end to end along the dimension named above; an argument that names none is the same for every part. Nothing has to cross between parts.
All inputs are finite; a program needn't handle non-finite values.
Results may differ from the reference program's by a relative error of at most 0.014.
Values may be sent and summed in bfloat16 or wider, within the bound.
A program may use at most 128 MiB of HBM per device.

```python
import math
import jax
import jax.numpy as jnp
from jax import lax

D = 4096
HEADS = 16
HEAD_DIM = 128
FF = 11264
BATCH = 8
N_TP = 2


def draw_tokens(key, part):
    key_base, key_rows, key_rough = jax.random.split(key, 3)
    ramp = jnp.exp(jnp.linspace(math.log(0.5), math.log(2.0), D)).reshape(1, D)
    rough = jax.random.uniform(key_rough, (1, D), jnp.float32, 0.5, 1.5)
    row_scale = jnp.exp(jax.random.uniform(key_rows, (BATCH, 1), jnp.float32, math.log(0.3), math.log(3.0)))
    base = jax.random.normal(key_base, (BATCH, D), jnp.float32)
    return jnp.clip(base * row_scale * ramp * rough, -16.0, 16.0).astype(jnp.bfloat16)


def strengthened(array, stream_key, source, target, blocks, factor):
    owner, partner = [(jnp.arange(array.shape[dim]) // (array.shape[dim] // blocks)).reshape([-1 if axis == dim else 1 for axis in range(array.ndim)]) for dim in (source, target)]
    chosen = jax.random.permutation(stream_key, blocks)[partner]
    strong = (owner == chosen) | (owner == (partner + blocks // 2) % blocks)
    return jnp.where(strong, factor * array, array)


def block_levels(stream_key, extent, cuts, least, largest):
    loudness, own = 1.0, jax.random.fold_in(stream_key, 6)
    for position, blocks in cuts:
        steps = jnp.exp(jax.random.uniform(jax.random.fold_in(own, position), (blocks,), jnp.float32, least / len(cuts), largest / len(cuts)))
        loudness = loudness * jnp.repeat(steps, extent[position] // blocks).reshape([-1 if axis == position else 1 for axis in range(len(extent))])
    return loudness


def scatter_about(rng, shape, spread, limit, cuts=(), held_as=jnp.bfloat16):
    array = jax.random.normal(rng, shape, jnp.float32) * spread
    if len(cuts) > 0:
        array = block_levels(rng, shape, cuts, -0.22, 0.18) * array
    return jnp.clip(array, min=-limit, max=limit).astype(held_as)


def gaussian_with(own_key, shape, width, reach, cuts, heavy, dtype=jnp.bfloat16):
    drawn = width * jax.random.normal(own_key, shape, jnp.float32)
    if cuts:
        drawn = drawn * block_levels(own_key, shape, cuts, -0.22, 0.18)
    return jnp.clip(strengthened(drawn, jax.random.fold_in(own_key, 3), *heavy), -reach, reach).astype(dtype)


def setup_inputs(seed: int = 0, part: int = 0) -> dict:
    arg_keys = jax.random.split(jax.random.key(seed), 18)
    part_splits = jax.random.split(jax.random.fold_in(arg_keys[17], part), 18)
    return {
        "tokens": draw_tokens(jax.random.fold_in(jax.random.fold_in(arg_keys[17], part), 71), part),
        "gain_mix": jnp.clip(1.0 + 0.18 * jax.random.normal(arg_keys[1], (D,), jnp.float32), 0.1, 1.9),
        "w_query": scatter_about(arg_keys[2], (D, HEADS * HEAD_DIM), D ** -0.5, 0.09375, ((0, 4), (1, 2))),
        "w_key": scatter_about(arg_keys[3], (D, HEADS * HEAD_DIM), D ** -0.5, 0.09375, ((0, 4), (1, 2))),
        "w_value": scatter_about(arg_keys[4], (D, HEADS * HEAD_DIM), D ** -0.5, 0.09375, ((0, 4), (1, 2))),
        "w_igate": scatter_about(arg_keys[5], (D, HEADS), D ** -0.5, 0.09375, ((0, 4), (1, 2))),
        "w_fgate": scatter_about(arg_keys[6], (D, HEADS), D ** -0.5, 0.09375, ((0, 4), (1, 2))),
        "bias_igate": jnp.clip(jax.random.uniform(arg_keys[7], (HEADS,), jnp.float32, -1.0, 1.0) * block_levels(arg_keys[7], (HEADS,), ((0, 2),), -0.4, 0.0), -1.0, 1.0),
        "bias_fgate": jnp.clip(-1.0 + 5.0 * jax.random.uniform(arg_keys[8], (HEADS,), jnp.float32) ** block_levels(arg_keys[8], (HEADS,), ((0, 2),), -0.2, 0.2), -1.0, 4.0),
        "memory": scatter_about(part_splits[9], (BATCH, HEADS, HEAD_DIM, HEAD_DIM), 0.1, 0.8, ((0, 4), (1, 2)), jnp.float32),
        "normalizer": scatter_about(part_splits[10], (BATCH, HEADS, HEAD_DIM), 0.1, 0.8, ((0, 4), (1, 2)), jnp.float32),
        "stabilizer": jnp.clip(jax.random.uniform(part_splits[11], (BATCH, HEADS), jnp.float32, -1.5, 1.5) * block_levels(part_splits[11], (BATCH, HEADS), ((0, 4), (1, 2)), -0.4, 0.0), -1.5, 1.5),
        "w_output": scatter_about(arg_keys[12], (HEADS * HEAD_DIM, D), (HEADS * HEAD_DIM) ** -0.5, 0.125, ((0, 2), (1, 4))),
        "gain_mlp": jnp.clip(1.0 + 0.18 * jax.random.normal(arg_keys[13], (D,), jnp.float32), 0.1, 1.9),
        "w_gate": scatter_about(arg_keys[14], (D, FF), D ** -0.5, 0.09375, ((1, 8),)),
        "w_up": scatter_about(arg_keys[15], (D, FF), D ** -0.5, 0.09375, ((1, 8),)),
        "w_down": gaussian_with(arg_keys[16], (FF, D), FF ** -0.5, 0.078125, ((0, 8),), (0, 1, 8, 2.0)),
    }


epsilon = 1e-06

def cell_update(queries, key_proj, values, in_gate, log_forget, memory, normalizer, stabilizer, head_count):
    batch_rows = queries.shape[0]
    query_heads = queries.astype(jnp.float32).reshape(batch_rows, head_count, -1)
    head_dim = query_heads.shape[2]
    key_heads = key_proj.astype(jnp.float32).reshape(batch_rows, head_count, head_dim) * head_dim ** (-0.5)
    value_heads = values.astype(jnp.float32).reshape(batch_rows, head_count, head_dim)
    stab_next = jnp.maximum(stabilizer + log_forget, in_gate)
    keeping = jnp.exp(stabilizer + log_forget - stab_next)
    fresh_weight = jnp.exp(in_gate - stab_next)
    memory_next = keeping[:, :, None, None] * memory + fresh_weight[:, :, None, None] * value_heads[:, :, :, None] * key_heads[:, :, None, :]
    norm_next = keeping[:, :, None] * normalizer + fresh_weight[:, :, None] * key_heads
    numerator = jnp.einsum('bhvk,bhk->bhv', memory_next, query_heads, precision=lax.Precision.HIGHEST)
    denominator = jnp.einsum('bhk,bhk->bh', norm_next, query_heads, precision=lax.Precision.HIGHEST)
    denominator = jnp.maximum(jnp.abs(denominator), jnp.exp(-stab_next))
    hidden = (numerator / denominator[:, :, None]).reshape(batch_rows, -1).astype(jnp.bfloat16)
    return (hidden, memory_next, norm_next, stab_next)

def reference(tokens, gain_mix, w_query, w_key, w_value, w_igate, w_fgate, bias_igate, bias_fgate, memory, normalizer, stabilizer, w_output, gain_mlp, w_gate, w_up, w_down):
    tok_float = tokens.astype(jnp.float32)
    scaling = lax.rsqrt(lax.optimization_barrier(jnp.mean(tok_float * tok_float, axis=1, keepdims=True)) + epsilon)
    scaled = (tok_float * gain_mix).astype(jnp.bfloat16)

    def project(weight):
        return scaling * jnp.dot(scaled, weight, preferred_element_type=jnp.float32)
    queries = project(w_query).astype(jnp.bfloat16)
    key_proj = project(w_key).astype(jnp.bfloat16)
    values = project(w_value).astype(jnp.bfloat16)
    in_gate = project(w_igate) + bias_igate
    log_forget = jax.nn.log_sigmoid(project(w_fgate) + bias_fgate)
    hidden, memory_next, norm_next, stab_next = cell_update(queries, key_proj, values, in_gate, log_forget, memory, normalizer, stabilizer, HEADS)
    block_cols = w_output.shape[0] // N_TP
    branch = jnp.zeros(tokens.shape, jnp.float32)
    for block_index in range(N_TP):
        lower = block_index * block_cols
        partial_out = jnp.dot(hidden[:, lower:lower + block_cols], w_output[lower:lower + block_cols], preferred_element_type=jnp.float32)
        rounded = lax.optimization_barrier(partial_out.astype(jnp.bfloat16))
        branch = branch + rounded.astype(jnp.float32)
    residual = (tok_float + branch).astype(jnp.bfloat16)
    res_float = residual.astype(jnp.float32)
    scaling_mlp = lax.rsqrt(lax.optimization_barrier(jnp.mean(res_float * res_float, axis=1, keepdims=True)) + epsilon)
    normed = (res_float * scaling_mlp * gain_mlp).astype(jnp.bfloat16)
    gate_act = jnp.dot(normed, w_gate, preferred_element_type=jnp.float32)
    up_act = jnp.dot(normed, w_up, preferred_element_type=jnp.float32)
    activated = (jax.nn.silu(gate_act) * up_act).astype(jnp.bfloat16)
    mixed = (res_float + jnp.dot(activated, w_down, preferred_element_type=jnp.float32)).astype(jnp.bfloat16)
    return (mixed, memory_next, norm_next, stab_next)
```

```python
import jax
import jax.numpy as jnp
from jax import lax
from jax.experimental import pallas as pl
from jax.experimental.pallas import tpu as pltpu
from jax.sharding import PartitionSpec as P

D = 4096


epsilon = 1e-06


def cell_update(
    queries, key_proj, values, in_gate, log_forget, memory, normalizer, stabilizer, head_count
):
    batch_rows = queries.shape[0]
    query_heads = queries.astype(jnp.float32).reshape(batch_rows, head_count, -1)
    head_dim = query_heads.shape[2]
    key_heads = key_proj.astype(jnp.float32).reshape(
        batch_rows, head_count, head_dim
    ) * head_dim ** (-0.5)
    value_heads = values.astype(jnp.float32).reshape(batch_rows, head_count, head_dim)
    stab_next = jnp.maximum(stabilizer + log_forget, in_gate)
    keeping = jnp.exp(stabilizer + log_forget - stab_next)
    fresh_weight = jnp.exp(in_gate - stab_next)
    memory_next = (
        keeping[:, :, None, None] * memory
        + fresh_weight[:, :, None, None] * value_heads[:, :, :, None] * key_heads[:, :, None, :]
    )
    norm_next = keeping[:, :, None] * normalizer + fresh_weight[:, :, None] * key_heads
    numerator = jnp.einsum(
        "bhvk,bhk->bhv", memory_next, query_heads, precision=lax.Precision.HIGHEST
    )
    denominator = jnp.einsum("bhk,bhk->bh", norm_next, query_heads, precision=lax.Precision.HIGHEST)
    denominator = jnp.maximum(jnp.abs(denominator), jnp.exp(-stab_next))
    hidden = (numerator / denominator[:, :, None]).reshape(batch_rows, -1).astype(jnp.bfloat16)
    return (hidden, memory_next, norm_next, stab_next)


def mixer_block(residual, gain_mlp, w_gate, w_up, w_down):
    full_rows = lax.all_gather(residual, "kv", axis=1, tiled=True).astype(jnp.float32)
    scaling = lax.rsqrt(jnp.mean(full_rows * full_rows, axis=1, keepdims=True) + epsilon)
    normed = (full_rows * scaling * gain_mlp).astype(jnp.bfloat16)
    gate_act = jnp.dot(normed, w_gate, preferred_element_type=jnp.float32)
    up_act = jnp.dot(normed, w_up, preferred_element_type=jnp.float32)
    activated = (jax.nn.silu(gate_act) * up_act).astype(jnp.bfloat16)
    down_terms = jnp.dot(activated, w_down, preferred_element_type=jnp.float32)
    return lax.psum_scatter(down_terms, ("kv", "tp"), scatter_dimension=1, tiled=True)


def local_plain(
    tokens,
    gain_mix,
    w_query,
    w_key,
    w_value,
    w_igate,
    w_fgate,
    bias_igate,
    bias_fgate,
    memory,
    normalizer,
    stabilizer,
    w_output,
    gain_mlp,
    w_gate,
    w_up,
    w_down,
):
    tok_float = tokens.astype(jnp.float32)
    scaled = (tok_float * gain_mix).astype(jnp.bfloat16)
    part_squares = jnp.sum(tok_float * tok_float, axis=1)
    query_part = jnp.dot(scaled, w_query, preferred_element_type=jnp.float32)
    key_part = jnp.dot(scaled, w_key, preferred_element_type=jnp.float32)
    value_part = jnp.dot(scaled, w_value, preferred_element_type=jnp.float32)
    igate_part = jnp.dot(scaled, w_igate, preferred_element_type=jnp.float32)
    fgate_part = jnp.dot(scaled, w_fgate, preferred_element_type=jnp.float32)
    query_sum, key_sum, value_sum, igate_sum, fgate_sum, own_squares = (
        lax.psum_scatter(query_part, "kv", scatter_dimension=0, tiled=True),
        lax.psum_scatter(key_part, "kv", scatter_dimension=0, tiled=True),
        lax.psum_scatter(value_part, "kv", scatter_dimension=0, tiled=True),
        lax.psum_scatter(igate_part, "kv", scatter_dimension=0, tiled=True),
        lax.psum_scatter(fgate_part, "kv", scatter_dimension=0, tiled=True),
        lax.psum_scatter(part_squares, "kv", scatter_dimension=0, tiled=True),
    )
    scaling = lax.rsqrt(own_squares / D + epsilon)[:, None]
    queries = (scaling * query_sum).astype(jnp.bfloat16)
    key_proj = (scaling * key_sum).astype(jnp.bfloat16)
    values = (scaling * value_sum).astype(jnp.bfloat16)
    in_gate = scaling * igate_sum + bias_igate
    log_forget = jax.nn.log_sigmoid(scaling * fgate_sum + bias_fgate)
    hidden, memory_next, norm_next, stab_next = cell_update(
        queries,
        key_proj,
        values,
        in_gate,
        log_forget,
        memory,
        normalizer,
        stabilizer,
        memory.shape[1],
    )
    branch_part = jnp.dot(
        lax.all_gather(hidden, "kv", axis=0, tiled=True),
        w_output,
        preferred_element_type=jnp.float32,
    )
    branch = lax.psum(branch_part.astype(jnp.bfloat16), "tp").astype(jnp.float32)
    residual = (tok_float + branch).astype(jnp.bfloat16)
    mixed_terms = mixer_block(residual, gain_mlp, w_gate, w_up, w_down)
    columns = mixed_terms.shape[1]
    residual_own = lax.dynamic_slice_in_dim(residual, lax.axis_index("tp") * columns, columns, 1)
    mixed = (residual_own.astype(jnp.float32) + mixed_terms).astype(jnp.bfloat16)
    return (mixed, memory_next, norm_next, stab_next)


SUBLANES, LANES = 8, 128
MESH = pl.DeviceIdType.MESH
NT = (((1,), (1,)), ((), ()))


def fused_kernel(
    n_kv,
    n_tp,
    tok_h, gmix_h, wq_h, wk_h, wv_h, wig_h, wfg_h, big_h, bfg_h, mem_h, nrm_h, stb_h,
    wo_h, gmlp_h, wg_h, wu_h, wd_h,
    mixed_h, memn_h, nrmn_h, stbn_h,
    tok, gmix, wqkv, wig, wfg, big, bfg, mem, nrm, stb, wo, gmlp, wg, wu, wd,
    memn, nrmn, stbn, mixed,
    mhi, mlo, scaled_pad,
    part_send, part_recv, gate_send, gate_recv, cells, hid_send, hid, br_send, br_recv,
    res, down_send, down_recv,
    in_sem, out_sem, wg_sem, wu_sem, wd_sem,
    send_sem, recv_sem,
):
    f32, bf16 = jnp.float32, jnp.bfloat16
    kv, tp, dp = lax.axis_index("kv"), lax.axis_index("tp"), lax.axis_index("dp")
    rows, width = tok.shape
    seqs, heads, hd = nrm.shape
    inner = heads * hd
    model = width * n_kv
    own_cols = mixed.shape[1]
    n_dev = n_kv * n_tp

    def peer(j, s):
        return lax.rem(kv + j, n_kv), lax.rem(tp + s, n_tp)

    others = [(j, s) for j in range(n_kv) for s in range(n_tp) if (j, s) != (0, 0)]
    dest_order = sorted(
        others, key=lambda js: (-min(js[0], n_kv - js[0]), js[0], js[1])
    ) + [(0, 0)]

    loads = {}

    def load(name, src, dst, sem):
        loads[name] = pltpu.make_async_copy(src, dst, sem)
        loads[name].start()

    small = [
        ("tok", tok_h, tok), ("gmix", gmix_h, gmix), ("wig", wig_h, wig), ("wfg", wfg_h, wfg),
        ("wq", wq_h, wqkv.at[0]), ("wk", wk_h, wqkv.at[1]), ("wv", wv_h, wqkv.at[2]),
        ("big", big_h, big), ("bfg", bfg_h, bfg), ("nrm", nrm_h, nrm), ("stb", stb_h, stb),
        ("mem", mem_h, mem), ("gmlp", gmlp_h, gmlp), ("wo", wo_h, wo),
    ]
    for i, (name, src, dst) in enumerate(small):
        load(name, src, dst, in_sem.at[i])
    for j in range(n_kv):
        src = lax.rem(kv + n_kv - j, n_kv)
        rng = pl.ds(pl.multiple_of(src * width, width), width)
        load(f"wg{j}", wg_h.at[rng, :], wg.at[j], wg_sem.at[j])
        load(f"wu{j}", wu_h.at[rng, :], wu.at[j], wu_sem.at[j])
    for i, (j, s) in enumerate(dest_order):
        dk, dt = peer(j, s)
        rng = pl.ds(pl.multiple_of((dk * n_tp + dt) * own_cols, own_cols), own_cols)
        load(f"wd{i}", wd_h.at[:, rng], wd.at[i], wd_sem.at[i])

    barrier = pltpu.get_barrier_semaphore()
    for j, s in others:
        dk, dt = peer(j, s)
        pl.semaphore_signal(barrier, inc=1, device_id=(dp, dk, dt), device_id_type=MESH)

    count = [0]
    sends = []

    def send(src, dst, j, s):
        i = count[0]
        count[0] += 1
        dk, dt = peer(j, s)
        copy = pltpu.make_async_remote_copy(
            src_ref=src, dst_ref=dst, send_sem=send_sem.at[i], recv_sem=recv_sem.at[i],
            device_id=(dp, dk, dt), device_id_type=MESH,
        )
        copy.start()
        sends.append(copy)
        return copy

    loads["tok"].wait()
    loads["gmix"].wait()
    tokf = tok[...].astype(f32)
    scaled = (tokf * gmix[...]).astype(bf16)
    scaled_pad[...] = jnp.zeros_like(scaled_pad)
    scaled_pad[0:rows, :] = scaled
    loads["wig"].wait()
    loads["wfg"].wait()
    padded = scaled_pad[...]
    ig = lax.dot_general(wig[...], padded, NT, preferred_element_type=f32)
    fg = lax.dot_general(wfg[...], padded, NT, preferred_element_type=f32)
    squares = jnp.sum(tokf * tokf, axis=1, keepdims=True)
    lane = lax.broadcasted_iota(jnp.int32, (rows, LANES), 1)
    row = lax.broadcasted_iota(jnp.int32, (rows, LANES), 0)
    square_row = jnp.sum(jnp.where(lane == row + 2 * rows, squares, 0.0), axis=0, keepdims=True)
    gates_own = ig + pltpu.roll(fg, rows, 1) + square_row
    gate_send[...] = gates_own

    for i, name in enumerate(("wq", "wk", "wv")):
        loads[name].wait()
        part = jnp.dot(scaled, wqkv[i], preferred_element_type=f32)
        for c in range(n_kv):
            part_send[c, :, i * inner : (i + 1) * inner] = part[c * seqs : (c + 1) * seqs, :]

    pl.semaphore_wait(barrier, n_dev - 1)
    hops = sorted(range(1, n_kv), key=lambda j: (-min(j, n_kv - j), j))
    gate_copies, part_copies = {}, {}
    for j in hops:
        dk, _ = peer(j, 0)
        part_copies[j] = send(part_send.at[dk], part_recv.at[j - 1], j, 0)
        gate_copies[j] = send(gate_send, gate_recv.at[j - 1], j, 0)

    loads["mem"].wait()
    for b in range(seqs):
        for h in range(heads):
            piece = mem[b, h]
            high = piece.astype(bf16)
            mhi[b, h * hd : (h + 1) * hd, :] = high
            mlo[b, h * hd : (h + 1) * hd, :] = (piece - high.astype(f32)).astype(bf16)
    for name in ("big", "bfg", "nrm", "stb"):
        loads[name].wait()
    eye = lax.broadcasted_iota(jnp.int32, (heads, heads), 0) == lax.broadcasted_iota(
        jnp.int32, (heads, heads), 1
    )

    def column(row_value):
        return jnp.sum(jnp.where(eye, row_value, 0.0), axis=1, keepdims=True)

    def as_row(column_value):
        return jnp.sum(jnp.where(eye, column_value, 0.0), axis=0, keepdims=True)

    bias_i = column(big[...])
    bias_f = column(bfg[...])
    block_of = lax.broadcasted_iota(jnp.int32, (heads, inner), 1) // hd
    head_of = lax.broadcasted_iota(jnp.int32, (heads, inner), 0)

    total = part_send[kv]
    gates = gates_own
    for j in hops:
        gate_copies[j].wait_recv()
        gates += gate_recv[j - 1]
    for j in hops:
        part_copies[j].wait_recv()
        total += part_recv[j - 1]
    for b in range(seqs):
        for i in range(3 * heads):
            cells[b, i : i + 1, :] = total[b : b + 1, i * hd : (i + 1) * hd]
    keeps, freshes = [], []
    for b in range(seqs):
        at = kv * seqs + b

        def pick(offset):
            return jnp.sum(jnp.where(lane == at + offset, gates, 0.0), axis=1, keepdims=True)

        scale = lax.rsqrt(pick(2 * rows) / model + epsilon)
        in_gate = scale * pick(0) + bias_i
        forget_in = scale * pick(rows) + bias_f
        log_forget = jnp.minimum(forget_in, 0.0) - jnp.log1p(jnp.exp(-jnp.abs(forget_in)))
        held = column(stb[b : b + 1, :]) + log_forget
        stab = jnp.maximum(held, in_gate)
        keep = jnp.exp(held - stab)
        fresh = jnp.exp(in_gate - stab)
        stbn[b : b + 1, :] = as_row(stab)
        query = (scale * cells[b, 0:heads, :]).astype(bf16)
        key = (scale * cells[b, heads : 2 * heads, :]).astype(bf16).astype(f32) * hd ** (-0.5)
        fresh_key = fresh * key
        cells[b, heads : 2 * heads, :] = fresh_key
        value = (scale * cells[b, 2 * heads :, :]).astype(bf16).astype(f32)
        cells[b, 2 * heads :, :] = value
        queryf = query.astype(f32)
        norm_next = keep * nrm[b] + fresh_key
        nrmn[b] = norm_next
        den = jnp.sum(norm_next * queryf, axis=1, keepdims=True)
        den = jnp.maximum(jnp.abs(den), jnp.exp(-stab))
        weight = jnp.sum(fresh_key * queryf, axis=1, keepdims=True)
        held_part = lax.dot_general(query, mhi[b], NT, preferred_element_type=f32)
        held_part += lax.dot_general(query, mlo[b], NT, preferred_element_type=f32)
        value_row = (scale[0:1, :] * total[b : b + 1, 2 * inner :]).astype(bf16).astype(f32)
        grid = (keep * held_part + weight * value_row) / den
        hid_send[b : b + 1, :] = jnp.sum(
            jnp.where(block_of == head_of, grid, 0.0), axis=0, keepdims=True
        )
        keeps.append(keep)
    hid_first = count[0]
    for j in hops:
        send(hid_send, hid.at[kv], j, 0)
    hid[kv] = hid_send[...]

    outs = []

    def store(src, dst):
        copy = pltpu.make_async_copy(src, dst, out_sem.at[len(outs)])
        copy.start()
        outs.append(copy)

    for b in range(seqs):
        value_t = cells[b, 2 * heads :, :].T
        for h in range(heads):
            memn[b, h] = (
                keeps[b][h : h + 1, :] * mem[b, h]
                + value_t[:, h : h + 1] * cells[b, heads + h : heads + h + 1, :]
            )

    loads["wo"].wait()
    for i, j in enumerate(hops):
        dk, dt = peer(j, 0)
        pltpu.make_async_remote_copy(
            src_ref=hid_send, dst_ref=hid.at[lax.rem(kv + n_kv - j, n_kv)],
            send_sem=send_sem.at[hid_first + i], recv_sem=recv_sem.at[hid_first + i],
            device_id=(dp, dk, dt), device_id_type=MESH,
        ).wait_recv()
    hidden = jnp.concatenate([hid[c] for c in range(n_kv)], axis=0).astype(bf16)
    branch = jnp.dot(hidden, wo[...], preferred_element_type=f32).astype(bf16)
    br_send[...] = branch
    partner_copies = [send(br_send, br_recv.at[s - 1], 0, s) for s in range(1, n_tp)]
    store(memn, memn_h)
    store(nrmn, nrmn_h)
    store(stbn, stbn_h)
    for copy in partner_copies:
        copy.wait_recv()
    branch_sum = branch.astype(f32)
    for s in range(1, n_tp):
        branch_sum += br_recv[s - 1].astype(f32)
    res[0] = (tokf + branch_sum).astype(bf16)
    res_copies = {j: send(res.at[0], res.at[j], j, 0) for j in hops}

    loads["gmlp"].wait()
    near = [0] + sorted(range(1, n_kv), key=lambda j: (min(j, n_kv - j), j))
    sums = jnp.zeros((rows, 1), f32)
    gate_acc = jnp.zeros((rows, wg.shape[2]), f32)
    up_acc = jnp.zeros((rows, wg.shape[2]), f32)
    for j in near:
        loads[f"wg{j}"].wait()
        loads[f"wu{j}"].wait()
        if j:
            res_copies[j].wait_recv()
        chunk = res[j].astype(f32)
        src_kv = lax.rem(kv + n_kv - j, n_kv)
        sums += jnp.sum(chunk * chunk, axis=1, keepdims=True)
        lhs = (chunk * gmlp[src_kv]).astype(bf16)
        gate_acc += jnp.dot(lhs, wg[j], preferred_element_type=f32)
        up_acc += jnp.dot(lhs, wu[j], preferred_element_type=f32)
    scale = lax.rsqrt(sums / model + epsilon)
    gate = scale * gate_acc
    activated = (gate * jax.nn.sigmoid(gate) * (scale * up_acc)).astype(bf16)

    down_copies = []
    own = None
    for i, (j, s) in enumerate(dest_order):
        loads[f"wd{i}"].wait()
        block = jnp.dot(activated, wd[i], preferred_element_type=f32)
        if (j, s) == (0, 0):
            own = block
        else:
            down_send[i] = block
            down_copies.append(send(down_send.at[i], down_recv.at[i], j, s))
    mine = pl.ds(pl.multiple_of(tp * own_cols, own_cols), own_cols)
    for i, copy in enumerate(down_copies):
        copy.wait_recv()
        own += down_recv[i]
    mixed[...] = (res[0, :, mine].astype(f32) + own).astype(bf16)
    store(mixed, mixed_h)
    for copy in sends:
        copy.wait_send()
    for copy in outs:
        copy.wait()


def fused(
    n_kv, n_tp,
    tokens, gain_mix, w_query, w_key, w_value, w_igate, w_fgate, bias_igate, bias_fgate,
    memory, normalizer, stabilizer, w_output, gain_mlp, w_gate, w_up, w_down,
):
    f32, bf16 = jnp.float32, jnp.bfloat16
    rows, width = tokens.shape
    seqs, heads, hd = normalizer.shape
    inner = heads * hd
    units = w_gate.shape[1]
    n_dev = n_kv * n_tp
    own_cols = width // n_tp
    copies = 4 * (n_kv - 1) + (n_tp - 1) + (n_dev - 1)
    anyspec = pl.BlockSpec(memory_space=pl.ANY)
    dma = pltpu.SemaphoreType.DMA
    out_shape = (
        jax.ShapeDtypeStruct((rows, own_cols), bf16),
        jax.ShapeDtypeStruct(memory.shape, f32),
        jax.ShapeDtypeStruct(normalizer.shape, f32),
        jax.ShapeDtypeStruct(stabilizer.shape, f32),
    )
    scratch = [
        pltpu.VMEM((rows, width), bf16),
        pltpu.VMEM((1, width), f32),
        pltpu.VMEM((3, width, inner), bf16),
        pltpu.VMEM((heads, width), bf16),
        pltpu.VMEM((heads, width), bf16),
        pltpu.VMEM((1, heads), f32),
        pltpu.VMEM((1, heads), f32),
        pltpu.VMEM(memory.shape, f32),
        pltpu.VMEM(normalizer.shape, f32),
        pltpu.VMEM(stabilizer.shape, f32),
        pltpu.VMEM((inner, width), bf16),
        pltpu.VMEM((n_kv, 1, width), f32),
        pltpu.VMEM((n_kv, width, units), bf16),
        pltpu.VMEM((n_kv, width, units), bf16),
        pltpu.VMEM((n_dev, units, own_cols), bf16),
        pltpu.VMEM(memory.shape, f32),
        pltpu.VMEM(normalizer.shape, f32),
        pltpu.VMEM(stabilizer.shape, f32),
        pltpu.VMEM((rows, own_cols), bf16),
        pltpu.VMEM((seqs, inner, hd), bf16),
        pltpu.VMEM((seqs, inner, hd), bf16),
        pltpu.VMEM((LANES, width), bf16),
        pltpu.VMEM((n_kv, seqs, 3 * inner), f32),
        pltpu.VMEM((n_kv - 1, seqs, 3 * inner), f32),
        pltpu.VMEM((heads, LANES), f32),
        pltpu.VMEM((n_kv - 1, heads, LANES), f32),
        pltpu.VMEM((seqs, 3 * heads, hd), f32),
        pltpu.VMEM((seqs, inner), f32),
        pltpu.VMEM((n_kv, seqs, inner), f32),
        pltpu.VMEM((rows, width), bf16),
        pltpu.VMEM((n_tp - 1, rows, width), bf16),
        pltpu.VMEM((n_kv, rows, width), bf16),
        pltpu.VMEM((n_dev, rows, own_cols), f32),
        pltpu.VMEM((n_dev - 1, rows, own_cols), f32),
        dma((14,)),
        dma((4,)),
        dma((n_kv,)),
        dma((n_kv,)),
        dma((n_dev,)),
        dma((copies,)),
        dma((copies,)),
    ]

    def body(*refs):
        fused_kernel(n_kv, n_tp, *refs)

    return pl.pallas_call(
        body,
        out_shape=out_shape,
        in_specs=[anyspec] * 17,
        out_specs=(anyspec,) * 4,
        scratch_shapes=scratch,
        compiler_params=pltpu.CompilerParams(
            collective_id=0, has_side_effects=True, vmem_limit_bytes=62 * 2**20
        ),
    )(
        tokens, gain_mix.reshape(1, width), w_query, w_key, w_value, w_igate.T, w_fgate.T,
        bias_igate.reshape(1, heads), bias_fgate.reshape(1, heads), memory, normalizer, stabilizer,
        w_output, gain_mlp.reshape(n_kv, 1, width), w_gate, w_up, w_down,
    )


def fits(n_kv, n_tp, tokens, normalizer, w_gate):
    rows, width = tokens.shape
    seqs, heads, hd = normalizer.shape
    units = w_gate.shape[1]
    weights = 2 * width * (4 * heads * hd + 3 * units * n_kv) + 16 * seqs * heads * hd * hd
    return (
        n_kv > 1
        and n_tp > 1
        and rows == SUBLANES
        and heads == SUBLANES
        and hd == LANES
        and seqs * n_kv == rows
        and width % (n_tp * LANES) == 0
        and units % LANES == 0
        and weights < 58 * 2**20
    )


def solution(mesh):
    n_kv, n_tp = mesh.shape["kv"], mesh.shape["tp"]

    def local(*args):
        tokens, normalizer, w_gate = args[0], args[10], args[14]
        if fits(n_kv, n_tp, tokens, normalizer, w_gate):
            return fused(n_kv, n_tp, *args)
        return local_plain(*args)

    placed = (
        P("dp", "kv"),
        P("kv"),
        P("kv", "tp"),
        P("kv", "tp"),
        P("kv", "tp"),
        P("kv", "tp"),
        P("kv", "tp"),
        P("tp"),
        P("tp"),
        P(("dp", "kv"), "tp", None, None),
        P(("dp", "kv"), "tp", None),
        P(("dp", "kv"), "tp"),
        P("tp", "kv"),
        P(),
        P(None, ("kv", "tp")),
        P(None, ("kv", "tp")),
        P(("kv", "tp"), None),
    )
    return jax.shard_map(
        local,
        mesh=mesh,
        in_specs=placed,
        out_specs=(
            P("dp", ("kv", "tp")),
            P(("dp", "kv"), "tp", None, None),
            P(("dp", "kv"), "tp", None),
            P(("dp", "kv"), "tp"),
        ),
        check_vma=False,
    )
```
